32 devices in a mesh: sp: 4 (over z), dp: 8 (over y, x, core).
Axes of the slice: x: 2, y: 2, z: 4, core: 2. Of those that a mesh axis runs over, the one named last changes fastest.
Arguments:
- hidden: bfloat16 [8, 512, 2048], P('dp', 'sp'), may hold values from -6 to 6
- queries: bfloat16 [8, 512, 1024], P('dp', 'sp'), may hold values from -6 to 6
- values: bfloat16 [8, 512, 2048], P('dp', 'sp'), may hold values from -6 to 6
- key_weight: bfloat16 [2048, 1024], P('dp'), may hold values from -0.125 to 0.125
- decay_down: bfloat16 [2048, 16], replicated, may hold values from -0.125 to 0.125
- decay_up: float32 [16, 1024], replicated, may hold values from -1.5 to 1.5
- decay_bias: float32 [1024], replicated, may hold values from -1 to 8
- span_shift: bfloat16 [8, 512], P('dp', 'sp'), may hold values from -1.5 to 1.5, as said below
- norm_gain: float32 [2048], replicated, may hold values from 0.1 to 1.9
Outputs:
- attended: bfloat16 [8, 512, 2048], P('dp', 'sp')
The draws below stay inside these ranges and needn't reach their ends.
Inputs may be any that keep to these rules, and one draw needn't show every extreme that they name: `span_shift`: constant over each aligned block of 64 positions.
All inputs are finite; a program needn't handle non-finite values.
Results may differ from the reference program's by a relative error of at most 0.0073.
Values may be sent and summed in bfloat16 or wider, within the bound.
A program may use at most 64 MiB of HBM per device.

```python
import jax
import jax.numpy as jnp
from jax import lax

D = 2048
HEADS = 4
DK = 256
DV = 512
RANK = 16
BLOCK = 64
KEY = 1024
VAL = 2048
LENGTH = 512
BATCH = 8


def draw_decay_bias(key, part):
    pick_key, slow_key, fast_key = jax.random.split(jax.random.fold_in(key, 11), 3)
    share = 5
    slow_pick = jax.random.randint(pick_key, (KEY,), 0, 10) < share
    slow_value = jax.random.uniform(slow_key, (KEY,), jnp.float32, 6.0, 8.0)
    fast_value = jax.random.uniform(fast_key, (KEY,), jnp.float32, -1.0, 0.5)
    return jnp.where(slow_pick, slow_value, fast_value).astype(jnp.float32)


def draw_span_shift(key, part):
    level_key, sign_key = jax.random.split(jax.random.fold_in(key, 23), 2)
    blocks = LENGTH // BLOCK
    levels = jax.random.uniform(level_key, (BATCH, blocks), jnp.float32, -1.5, 1.5)
    return jnp.repeat(levels, BLOCK, axis=1).astype(jnp.bfloat16)


def steps_of(key, shape, cuts, low, top_value):
    loudness, own = 1.0, jax.random.fold_in(key, 6)
    for dim, shards_of in cuts:
        heights = jnp.exp(jax.random.uniform(jax.random.fold_in(own, dim), (shards_of,), jnp.float32, low / len(cuts), top_value / len(cuts)))
        loudness = loudness * jnp.repeat(heights, shape[dim] // shards_of).reshape([-1 if axis == dim else 1 for axis in range(len(shape))])
    return loudness


def gaussian(own_key, shape, spread, reach, cuts=(), dtype=jnp.bfloat16):
    values = jax.random.normal(own_key, shape, jnp.float32) * spread
    if len(cuts) > 0:
        values = steps_of(own_key, shape, cuts, -0.22, 0.18) * values
    return jnp.clip(values, min=-reach, max=reach).astype(dtype)


def setup_inputs(seed: int = 0) -> dict:
    splits = jax.random.split(jax.random.key(seed), 10)
    hidden = gaussian(splits[0], (BATCH, LENGTH, D), 1.0, 6.0, ((0, 8), (1, 4)))
    queries = gaussian(splits[1], (BATCH, LENGTH, KEY), 1.0, 6.0, ((0, 8), (1, 4)))
    values = gaussian(splits[2], (BATCH, LENGTH, VAL), 1.0, 6.0, ((0, 8), (1, 4)))
    key_weight = gaussian(splits[3], (D, KEY), D ** -0.5, 0.125, ((0, 8),))
    decay_down = gaussian(splits[4], (D, RANK), D ** -0.5, 0.125)
    decay_up = gaussian(splits[5], (RANK, KEY), RANK ** -0.5, 1.5, (), jnp.float32)
    decay_bias = draw_decay_bias(jax.random.fold_in(splits[9], 71), 0)
    span_shift = draw_span_shift(jax.random.fold_in(splits[9], 71), 0)
    norm_gain = jnp.clip(1.0 + 0.18 * jax.random.normal(splits[8], (VAL,), jnp.float32), 0.1, 1.9)
    return dict(hidden=hidden, queries=queries, values=values, key_weight=key_weight, decay_down=decay_down, decay_up=decay_up, decay_bias=decay_bias, span_shift=span_shift, norm_gain=norm_gain)


decay_tau = 16.0
norm_eps = 1e-05
highest = lax.Precision.HIGHEST

def mechanism(query, keys_in, value_in, log_decay):
    length, key_width = query.shape
    value_width = value_in.shape[-1]
    blocks = length // BLOCK
    step_decay = log_decay.reshape(blocks, BLOCK, key_width)
    inclusive = jnp.cumsum(step_decay, axis=1)
    exclusive = inclusive - step_decay
    total = inclusive[:, -1, :]
    query3 = query.reshape(blocks, BLOCK, key_width)
    keys3 = keys_in.reshape(blocks, BLOCK, key_width)
    value_tensor3 = value_in.reshape(blocks, BLOCK, value_width)
    query_forward_part = (query3 * jnp.exp(inclusive)).astype(jnp.bfloat16)
    key_fwd = (keys3 * jnp.exp(-inclusive)).astype(jnp.bfloat16)
    query_reverse_part = (query3 * jnp.exp(-exclusive)).astype(jnp.bfloat16)
    key_bwd = (keys3 * jnp.exp(exclusive)).astype(jnp.bfloat16)
    key_end = (keys3 * jnp.exp(total[:, None, :] - inclusive)).astype(jnp.bfloat16)
    fwd_scores = jnp.einsum('nid,njd->nij', query_forward_part, key_fwd, preferred_element_type=jnp.float32)
    bwd_scores = jnp.einsum('nid,njd->nij', query_reverse_part, key_bwd, preferred_element_type=jnp.float32)
    row_index = lax.broadcasted_iota(jnp.int32, (BLOCK, BLOCK), 0)
    col_index = lax.broadcasted_iota(jnp.int32, (BLOCK, BLOCK), 1)
    attention_scores = jnp.where((col_index <= row_index)[None], fwd_scores, bwd_scores).astype(jnp.bfloat16)
    inner_block_term = jnp.einsum('ucy,uyh->uch', attention_scores, value_tensor3, preferred_element_type=jnp.float32)
    end_terms = jnp.einsum('njd,nje->nde', key_end, value_tensor3, preferred_element_type=jnp.float32)
    start_terms = jnp.einsum('njd,nje->nde', key_bwd, value_tensor3, preferred_element_type=jnp.float32)
    rates = jnp.exp(total)

    def forward_step(carry_state, inputs):
        rate, term = inputs
        return (rate[:, None] * carry_state + term, carry_state)

    def backward_step(carry_state, inputs):
        rate, term = inputs
        state_here = rate[:, None] * carry_state
        return (state_here + term, state_here)
    empty = jnp.zeros((key_width, value_width), jnp.float32)
    _, forward_scan_states = lax.scan(forward_step, empty, (rates, end_terms))
    _, reverse_scan_states = lax.scan(backward_step, empty, (rates, start_terms), reverse=True)
    produced_rows = jnp.einsum('tzv,tvg->tzg', query_forward_part, forward_scan_states.astype(jnp.bfloat16), preferred_element_type=jnp.float32)
    produced_rows = produced_rows + jnp.einsum('tzv,tvg->tzg', query_reverse_part, reverse_scan_states.astype(jnp.bfloat16), preferred_element_type=jnp.float32)
    return (inner_block_term + produced_rows).reshape(length, value_width).astype(jnp.bfloat16)

def head_norm(mixed, gain):
    rows = mixed.shape[0]
    grouped = mixed.astype(jnp.float32).reshape(rows, HEADS, DV)
    normed = grouped * lax.rsqrt(lax.optimization_barrier(jnp.mean(grouped * grouped, axis=-1, keepdims=True)) + norm_eps)
    return (normed * gain.reshape(HEADS, DV)[None]).reshape(rows, VAL).astype(jnp.bfloat16)

def reference(hidden, queries, values, key_weight, decay_down, decay_up, decay_bias, span_shift, norm_gain):
    token_rows = hidden.reshape(-1, D)
    keys = jnp.dot(token_rows, key_weight, preferred_element_type=jnp.float32).astype(jnp.bfloat16).reshape(BATCH, LENGTH, KEY)
    low = jnp.dot(token_rows, decay_down, preferred_element_type=jnp.float32).astype(jnp.bfloat16).reshape(BATCH, LENGTH, RANK)

    def per_sequence(inputs):
        query_seq, keys_seq, value_seq, low_seq, shift_seq = inputs
        pre = jnp.dot(low_seq.astype(jnp.float32), decay_up, precision=highest, preferred_element_type=jnp.float32)
        pre = pre + decay_bias[None, :] + shift_seq.astype(jnp.float32)[:, None]
        log_decay = jax.nn.log_sigmoid(pre) / decay_tau

        def by_head(tensor, width):
            return tensor.reshape(LENGTH, HEADS, width).transpose(1, 0, 2)
        scaled = by_head(query_seq, DK).astype(jnp.float32) * DK ** (-0.5)
        mixed = jax.vmap(mechanism)(scaled, by_head(keys_seq, DK).astype(jnp.float32), by_head(value_seq, DV), by_head(log_decay, DK))
        return head_norm(mixed.transpose(1, 0, 2).reshape(LENGTH, VAL), norm_gain)
    return lax.map(per_sequence, (queries, keys, values, low, span_shift))
```

```python
import functools

import jax
import jax.numpy as jnp
from jax import lax
from jax.experimental import pallas as pl
from jax.experimental.pallas import tpu as pltpu
from jax.sharding import PartitionSpec as P

HEADS = 4
DK = 256
DV = 512
BLOCK = 64
KEY = 1024
VAL = 2048
CORES = 2
SPLIT = 4
DVS = DV // SPLIT
STATES = (0, 1)
PAIRS = (2, 3)
PLAN = (
    ("prep", 0), ("prep", 1), ("prep", 2), ("relay", 0), ("first", 1), ("rest", 1), ("first", 2),
    ("prep", 3), ("hand", 0), ("forward", 2), ("last", 0), ("wall", 0), ("project", 0), ("values", 1),
    ("queries", 0), ("queries", 1), ("forward", 3), ("relay", 1), ("rest", 2), ("first", 3),
    ("hand", 1), ("middle", 0), ("serve", 0), ("last", 1), ("wall", 1), ("project", 1), ("queries", 2),
    ("queries", 3), ("relay", 2), ("rest", 3), ("hand", 2), ("last", 2), ("middle", 1), ("relay", 3),
    ("wall", 2), ("project", 2), ("hand", 3), ("serve", 1), ("finish", 0), ("last", 3), ("wall", 3),
    ("project", 3), ("middle", 2), ("finish", 1), ("middle", 3), ("serve", 2), ("finish", 2),
    ("serve", 3), ("finish", 3),
)

decay_tau = 16.0
norm_eps = 1e-05
highest = lax.Precision.HIGHEST
MESH = pl.DeviceIdType.MESH
f32 = jnp.float32
bf16 = jnp.bfloat16


def each(low, high, fn):
    if high - low <= 4:
        for j in range(low, high):
            fn(j)
    else:
        lax.fori_loop(low, high, lambda j, c: (fn(j), c)[1], 0)


def dot_nt(a, b):
    return lax.dot_general(a, b, (((1,), (1,)), ((), ())), preferred_element_type=f32)


def dot_tn(a, b):
    return lax.dot_general(a, b, (((0,), (0,)), ((), ())), preferred_element_type=f32)


def kernel(
    n_sp, n_dp,
    hid, que, val, kw, down, up, bias, shift, gain,
    out,
    wbuf, hv, qv, vv, outv, qf, qb, qx, qs, fac, rate, local, sbuf, rbuf, acc,
    lsem, osem, wsend, wrecv, psend, precv, csend, crecv, dsend, drecv,
):
    sp = lax.axis_index("sp")
    dp = lax.axis_index("dp")
    chips = n_dp // CORES
    chip = dp // CORES
    core = dp % CORES
    partner = chip * CORES + (1 - core)
    tok = hv.shape[0]
    depth = kw.shape[0]

    square = chips == 4
    half = depth // 2

    def across(j):
        return (chip + 1 - 2 * lax.rem(chip, 2), lax.rem(chip + 2, 4), 3 - chip)[j - 1]

    def peer(j):
        if square:
            return across(j) * CORES + core
        return lax.rem(chip + j, chips) * CORES + core

    def source_chip(j):
        if square:
            return chip if j == 0 else across(j)
        return lax.rem(chip - j + chips, chips)

    wlocal = [
        pltpu.make_async_copy(kw.at[:, pl.ds(h * DK, DK)], wbuf.at[h, dp], lsem.at[h])
        for h in range(HEADS)
    ]
    inputs = [
        pltpu.make_async_copy(a, b, lsem.at[HEADS + i])
        for i, (a, b) in enumerate(((hid, hv), (que, qv), (val, vv)))
    ]
    for c in wlocal + inputs:
        c.start()

    barrier = pltpu.get_barrier_semaphore()
    each(1, chips, lambda j: pl.semaphore_signal(
        barrier, inc=1, device_id={"dp": peer(j)}, device_id_type=MESH))
    pl.semaphore_signal(barrier, inc=1, device_id={"dp": partner}, device_id_type=MESH)

    for side in (1, n_sp - 1):
        pl.semaphore_signal(
            barrier, inc=1, device_id={"sp": lax.rem(sp + side, n_sp)}, device_id_type=MESH)
    pl.semaphore_wait(barrier, chips + 2)

    def wcopy(h, j):
        return pltpu.make_async_remote_copy(
            src_ref=wbuf.at[h, dp], dst_ref=wbuf.at[h, dp],
            send_sem=wsend.at[h, j], recv_sem=wrecv.at[h, j],
            device_id={"dp": peer(j)}, device_id_type=MESH)

    def wland(h, j):
        slot = wbuf.at[h, source_chip(j) * CORES + core]
        return pltpu.make_async_remote_copy(
            src_ref=slot, dst_ref=slot,
            send_sem=wsend.at[h, j], recv_sem=wrecv.at[h, j],
            device_id={"dp": peer(j)}, device_id_type=MESH)

    def pcopy(h, j):
        slot = wbuf.at[h, source_chip(j) * CORES + core]
        return pltpu.make_async_remote_copy(
            src_ref=slot, dst_ref=slot,
            send_sem=psend.at[h, j], recv_sem=precv.at[h, j],
            device_id={"dp": partner}, device_id_type=MESH)

    def pland(h, j):
        slot = wbuf.at[h, source_chip(j) * CORES + (1 - core)]
        return pltpu.make_async_remote_copy(
            src_ref=slot, dst_ref=slot,
            send_sem=psend.at[h, j], recv_sem=precv.at[h, j],
            device_id={"dp": partner}, device_id_type=MESH)

    direct = 3 if square else chips

    def diagonal(h, i, lands):
        origin = source_chip(3) if lands else source_chip(1 + i)
        slot = wbuf.at[h, origin * CORES + core, pl.ds(i * half, half), :]
        return pltpu.make_async_remote_copy(
            src_ref=slot, dst_ref=slot,
            send_sem=dsend.at[h, i], recv_sem=drecv.at[h, i],
            device_id={"dp": peer(2 - i)}, device_id_type=MESH)

    def phase_send(h):
        wlocal[h].wait()
        each(1, direct, lambda j: wcopy(h, j).start())
        pcopy(h, 0).start()

    def phase_relay(h):
        def relay(j):
            wland(h, j).wait_recv()
            if square:
                diagonal(h, j - 1, False).start()
            pcopy(h, j).start()
        each(1, direct, relay)

    ahead = 2 if square else HEADS
    for h in range(ahead):
        phase_send(h)

    inputs[0].wait()
    low = dot_nt(hv[...], down[...]).astype(bf16)
    steps = shift[...].astype(f32)
    inputs[1].wait()
    row = lax.broadcasted_iota(jnp.int32, (tok, DK), 0)
    first = row < BLOCK
    ti = lax.broadcasted_iota(jnp.int32, (tok, tok), 0)
    tj = lax.broadcasted_iota(jnp.int32, (tok, tok), 1)
    same = (ti < BLOCK) == (tj < BLOCK)
    below = tj <= ti
    tri = jnp.where(same & below, 1.0, 0.0).astype(f32)
    def phase_prep(h):
        cols = pl.ds(h * DK, DK)
        pre = jnp.dot(low.astype(f32), up[:, cols], precision=highest, preferred_element_type=f32)
        pre = pre + bias[:, cols] + jnp.where(first, steps[:, :1], steps[:, BLOCK:BLOCK + 1])
        logd = (jnp.minimum(pre, 0.0) - jnp.log1p(jnp.exp(-jnp.abs(pre)))) * (1.0 / decay_tau)
        incl = jnp.dot(tri, logd, precision=highest, preferred_element_type=f32)
        excl = incl - logd
        t0 = incl[BLOCK - 1:BLOCK, :]
        t1 = incl[tok - 1:tok, :]
        here = jnp.where(first, t0, t1)
        after = jnp.where(first, t1, 0.0)
        before = jnp.where(first, 0.0, t0)
        scaled = qv[:, cols].astype(f32) * DK ** (-0.5)
        qf[:, cols] = (scaled * jnp.exp(incl)).astype(bf16)
        qb[:, cols] = (scaled * jnp.exp(-excl)).astype(bf16)
        qx[:, cols] = (scaled * jnp.exp(here - excl)).astype(bf16)
        qs[0, :, cols] = (scaled * jnp.exp(incl + before)).astype(bf16)
        qs[1, :, cols] = (scaled * jnp.exp(here - excl + after)).astype(bf16)
        fac[0, :, cols] = jnp.exp(-incl)
        fac[1, :, cols] = jnp.exp(excl)
        fac[2, :, cols] = jnp.exp(here - incl)
        fac[3, :, cols] = jnp.exp(here - incl + after)
        fac[4, :, cols] = jnp.exp(excl + before)
        rate[:, cols] = jnp.exp(t0 + t1)

    inputs[2].wait()

    def chain(way, h, s):
        target = jnp.clip(sp + 1 - 2 * way, 0, n_sp - 1)
        return pltpu.make_async_remote_copy(
            src_ref=sbuf.at[way, h, s], dst_ref=rbuf.at[way, h, s],
            send_sem=csend.at[way, h, s], recv_sem=crecv.at[way, h, s],
            device_id={"sp": target}, device_id_type=MESH)

    def phase_keys(h):
        if square:
            for i in range(2):
                diagonal(h, i, True).wait_recv()
            pcopy(h, 3).start()
        each(0, chips, lambda j: pland(h, j).wait_recv())
        cols = pl.ds(h * DK, DK)
        weights = wbuf[h].reshape(n_dp * depth, DK)
        keys = jnp.dot(hv[...], weights, preferred_element_type=f32).astype(bf16).astype(f32)
        v = vv[:, pl.ds(h * DV, DV)]
        k_fwd = (keys * fac[3, :, cols]).astype(bf16)
        k_bwd = (keys * fac[4, :, cols]).astype(bf16)
        for way, k in ((0, k_fwd), (1, k_bwd)):
            local[way, h] = dot_tn(v, k)

            @pl.when(sp == (0 if way == 0 else n_sp - 1))
            def _(way=way):
                for s in range(SPLIT):
                    sbuf[way, h, s] = local[way, h, pl.ds(s * DVS, DVS), :].astype(bf16)
                    chain(way, h, s).start()

        kf = (keys * fac[0, :, cols]).astype(bf16)
        kb = (keys * fac[1, :, cols]).astype(bf16)
        ke = (keys * fac[2, :, cols]).astype(bf16)
        query_f, query_b, query_x = qf[:, cols], qb[:, cols], qx[:, cols]
        lower = jnp.where(same, dot_nt(query_f, kf), dot_nt(query_f, ke))
        upper = jnp.where(same, dot_nt(query_b, kb), dot_nt(query_x, kb))
        scores = jnp.where(below, lower, upper).astype(bf16)
        acc[h] = jnp.dot(scores, v, preferred_element_type=f32)

    def phase_chain(way, h):
        cols = pl.ds(h * DK, DK)
        edge = way * (n_sp - 1)
        other = (1 - way) * (n_sp - 1)

        @pl.when(sp != edge)
        def _():
            for s in range(SPLIT):
                rows = pl.ds(s * DVS, DVS)
                chain(way, h, s).wait_recv()

                @pl.when(sp != other)
                def _(s=s, rows=rows):
                    state = rbuf[way, h, s].astype(f32) * rate[:, cols] + local[way, h, rows, :]
                    sbuf[way, h, s] = state.astype(bf16)
                    chain(way, h, s).start()

                acc[h, :, rows] += dot_nt(qs[way, :, cols], rbuf[way, h, s])

    def out_copy(h):
        cols = pl.ds(h * DV, DV)
        return pltpu.make_async_copy(outv.at[:, cols], out.at[:, cols], osem.at[h])

    def phase_out(h):
        cols = pl.ds(h * DV, DV)
        mixed = acc[h].astype(bf16).astype(f32)
        scale = lax.rsqrt(jnp.mean(mixed * mixed, axis=-1, keepdims=True) + norm_eps)
        outv[:, cols] = (mixed * scale * gain[:, cols]).astype(bf16)
        out_copy(h).start()

    near = jnp.where(sp * 2 < n_sp, 0, 1)
    far = 1 - near
    def relay_on(h):
        if h < HEADS:
            phase_relay(h)
            if h + ahead < HEADS:
                phase_send(h + ahead)

    def phase_near(h):
        phase_chain(near, h)

    def phase_far(h):
        phase_chain(far, h)
        phase_out(h)

    plan = ((phase_prep, 0), (relay_on, 0), (phase_prep, 1), (relay_on, 1), (phase_keys, 0), (phase_prep, 2), (relay_on, 2), (phase_keys, 1), (phase_prep, 3), (relay_on, 3), (phase_keys, 2), (phase_near, 0), (phase_keys, 3), (phase_near, 1), (phase_far, 0), (phase_near, 2), (phase_far, 1), (phase_near, 3), (phase_far, 2), (phase_far, 3))
    for phase, h in plan:
        phase(h)

    for h in range(HEADS):
        each(1, direct, lambda j, h=h: wcopy(h, j).wait_send())
        each(0, chips, lambda j, h=h: pcopy(h, j).wait_send())
        if square:
            for i in range(2):
                diagonal(h, i, False).wait_send()
        for way in range(2):
            @pl.when(sp != (1 - way) * (n_sp - 1))
            def _(h=h, way=way):
                for s in range(SPLIT):
                    chain(way, h, s).wait_send()
        out_copy(h).wait()


def line_kernel(
    n_sp, n_dp,
    hid, que, val, kw, down_in, up_in, bias_in, shift_in, gain_in,
    out,
    down, up, bias, shift, gain,
    wbuf, hv, qv, vcat, outv, qf, qb, qx, qs, fac, rate, acc, base,
    kcat, knear, q2, qraw, ke, vin, kin, sbuf, rbuf, obuf, oin,
    lsem, osem, wsend, wfirst, wrest, wdiag, wpart, zsend, zrecv,
):
    sp = lax.axis_index("sp")
    dp = lax.axis_index("dp")
    chip = dp // CORES
    core = dp % CORES
    partner = chip * CORES + (1 - core)
    tok = hv.shape[0]
    depth = kw.shape[0]
    half = depth // 2
    n_chips = n_dp // CORES

    side = sp // 2
    other = 1 - side
    mate = sp + 1 - 2 * lax.rem(sp, 2)
    across = n_sp - 1 - sp
    edge = (sp == 0) | (sp == n_sp - 1)
    inner = jnp.logical_not(edge)

    def chip_at(j):
        return (chip, chip + 1 - 2 * lax.rem(chip, 2), lax.rem(chip + 2, 4), 3 - chip)[j]

    def dev(j):
        return chip_at(j) * CORES + core

    wlocal = [
        pltpu.make_async_copy(kw.at[:, pl.ds(h * DK, DK)], wbuf.at[h, dp], lsem.at[h])
        for h in range(HEADS)
    ]
    loads = [
        pltpu.make_async_copy(a, b, lsem.at[HEADS + i])
        for i, (a, b) in enumerate((
            (hid, hv), (que, qv), (val, vcat.at[pl.ds(tok, tok)]),
            (down_in, down), (up_in, up), (bias_in, bias), (shift_in, shift), (gain_in, gain)))
    ]
    barrier = pltpu.get_barrier_semaphore()
    for j in (1, 2):
        pl.semaphore_signal(barrier, inc=1, device_id={"dp": dev(j)}, device_id_type=MESH)
    pl.semaphore_signal(barrier, inc=1, device_id={"dp": partner}, device_id_type=MESH)
    pl.semaphore_signal(barrier, inc=1, device_id={"sp": mate}, device_id_type=MESH)

    @pl.when(inner)
    def _():
        pl.semaphore_signal(barrier, inc=1, device_id={"sp": across}, device_id_type=MESH)

    wlocal[0].start()
    for i in (2, 0, 3, 4, 5, 6, 1):
        loads[i].start()
    for h in range(1, HEADS):
        wlocal[h].start()
    loads[7].start()
    pl.semaphore_wait(barrier, jnp.where(inner, 5, 4))

    def rows(i):
        return pl.ds(i * half, half)

    def wcopy(h, j, i):
        part = wbuf.at[h, dp, rows(i)]
        first = i == j - 1
        return pltpu.make_async_remote_copy(
            src_ref=part, dst_ref=part, send_sem=wsend.at[0],
            recv_sem=wfirst.at[h, i] if first else wrest.at[h],
            device_id={"dp": dev(j)}, device_id_type=MESH)

    def relay(h, i):
        part = wbuf.at[h, dev(1 + i), rows(i)]
        return pltpu.make_async_remote_copy(
            src_ref=part, dst_ref=part, send_sem=wsend.at[0], recv_sem=wdiag.at[h],
            device_id={"dp": dev(2 - i)}, device_id_type=MESH)

    def pcopy(h, j):
        slot = wbuf.at[h, dev(j)]
        return pltpu.make_async_remote_copy(
            src_ref=slot, dst_ref=slot, send_sem=wsend.at[0], recv_sem=wpart.at[h],
            device_id={"dp": partner}, device_id_type=MESH)

    def landed(ref, sem):
        pltpu.make_async_remote_copy(
            src_ref=ref, dst_ref=ref, send_sem=zsend.at[0], recv_sem=sem,
            device_id={"sp": mate}, device_id_type=MESH).wait_recv()

    def gone(ref, sem):
        pltpu.make_async_remote_copy(
            src_ref=ref, dst_ref=ref, send_sem=sem, recv_sem=zrecv.at[0],
            device_id={"sp": mate}, device_id_type=MESH).wait_send()

    def zput(src, dst, send, recv, target):
        pltpu.make_async_remote_copy(
            src_ref=src, dst_ref=dst, send_sem=zsend.at[send], recv_sem=zrecv.at[recv],
            device_id={"sp": target}, device_id_type=MESH).start()

    def wsend_first(h):
        wlocal[h].wait()
        for j in (1, 2):
            wcopy(h, j, j - 1).start()
        pcopy(h, 0).start()

    def wsend_rest(h):
        for j in (1, 2):
            wcopy(h, j, 2 - j).start()

    def wrelay(h):
        for i in range(2):
            landed(wbuf.at[h, dev(1 + i), rows(i)], wfirst.at[h, i])
            relay(h, i).start()

    def wpass(h):
        landed(wbuf.at[h, 0], wrest.at[h])
        for j in (1, 2):
            pcopy(h, j).start()

    def wlast(h):
        landed(wbuf.at[h, dev(3)], wdiag.at[h])
        pcopy(h, 3).start()

    def wall(h):
        landed(wbuf.at[h, pl.ds(0, n_chips)], wpart.at[h])

    VE, QE, KE = 0, HEADS, 2 * HEADS
    ST = 3 * HEADS
    VIN = ST + len(STATES) * SPLIT
    KIN = VIN + 2 * len(PAIRS)

    lo, hi = pl.ds(0, tok), pl.ds(tok, tok)

    def kcols(h):
        return pl.ds(h * DK, DK)

    def vcols(h):
        return pl.ds(h * DV, DV)

    def edge_values(h):
        @pl.when(edge)
        def _():
            zput(vcat.at[hi, vcols(h)], vcat.at[lo, vcols(h)], 0, VE + h, mate)

    def inner_values(h):
        @pl.when(inner)
        def _():
            zput(vcat.at[hi, vcols(h)], vin.at[PAIRS.index(h), lo], 0, VIN + 2 * PAIRS.index(h), across)

    def vforward(h):
        @pl.when(inner)
        def _():
            i = PAIRS.index(h)
            landed(vcat.at[lo, vcols(h)], zrecv.at[VE + h])
            zput(vcat.at[lo, vcols(h)], vin.at[i, hi], 0, VIN + 2 * i + 1, across)

    def edge_queries(h):
        @pl.when(edge)
        def _():
            zput(qs.at[other, h], qraw.at[h], 1, QE + h, mate)

    wsend_first(0)
    wsend_rest(0)
    loads[2].wait()
    for h in PAIRS:
        inner_values(h)
    for h in PAIRS + STATES[:1]:
        edge_values(h)

    for i in (0, 3):
        loads[i].wait()
    low = dot_nt(hv[...], down[...]).astype(bf16).astype(f32)
    for i in (4, 5, 6, 1):
        loads[i].wait()
    steps = shift[...].astype(f32)
    row = lax.broadcasted_iota(jnp.int32, (tok, DK), 0)
    first = row < BLOCK
    ti = lax.broadcasted_iota(jnp.int32, (tok, tok), 0)
    tj = lax.broadcasted_iota(jnp.int32, (tok, tok), 1)
    same = (ti < BLOCK) == (tj < BLOCK)
    below = tj <= ti
    tri = jnp.where(same & below, 1.0, 0.0).astype(f32)

    def prep(h):
        cols = kcols(h)
        pre = jnp.dot(low, up[:, cols], precision=highest, preferred_element_type=f32)
        pre = pre + bias[:, cols] + jnp.where(first, steps[:, :1], steps[:, BLOCK:BLOCK + 1])
        logd = (jnp.minimum(pre, 0.0) - jnp.log1p(jnp.exp(-jnp.abs(pre)))) * (1.0 / decay_tau)
        incl = jnp.dot(tri, logd, precision=highest, preferred_element_type=f32)
        excl = incl - logd
        t0 = incl[BLOCK - 1:BLOCK, :]
        t1 = incl[tok - 1:tok, :]
        here = jnp.where(first, t0, t1)
        after = jnp.where(first, t1, 0.0)
        before = jnp.where(first, 0.0, t0)
        scaled = qv[:, cols].astype(f32) * DK ** (-0.5)
        qf[:, cols] = (scaled * jnp.exp(incl)).astype(bf16)
        qb[:, cols] = (scaled * jnp.exp(-excl)).astype(bf16)
        qx[:, cols] = (scaled * jnp.exp(here - excl)).astype(bf16)
        qs[0, h] = (scaled * jnp.exp(incl + before)).astype(bf16)
        qs[1, h] = (scaled * jnp.exp(here - excl + after)).astype(bf16)
        fac[0, :, cols] = jnp.exp(-incl)
        fac[1, :, cols] = jnp.exp(excl)
        fac[2, :, cols] = jnp.exp(here - incl)
        fac[3, :, cols] = jnp.exp(here - incl + after)
        fac[4, :, cols] = jnp.exp(excl + before)
        rate[:, cols] = jnp.exp(t0 + t1)

    def project(h):
        cols = kcols(h)
        weights = wbuf[h].reshape(n_dp * depth, DK)
        keys = jnp.dot(hv[...], weights, preferred_element_type=f32).astype(bf16).astype(f32)
        kcat[h, hi] = (keys * fac[3 + side, :, cols]).astype(bf16)

        @pl.when(edge)
        def _():
            zput(kcat.at[h, hi], ke.at[h], 2, KE + h, mate)

        if h in PAIRS:
            @pl.when(inner)
            def _():
                i = PAIRS.index(h)
                zput(kcat.at[h, hi], kin.at[i, lo], 1, KIN + 2 * i, across)

        knear[h] = (keys * fac[3 + other, :, cols]).astype(bf16)
        v = vcat[hi, vcols(h)]
        kf = (keys * fac[0, :, cols]).astype(bf16)
        kb = (keys * fac[1, :, cols]).astype(bf16)
        kx = (keys * fac[2, :, cols]).astype(bf16)
        query_f, query_b, query_x = qf[:, cols], qb[:, cols], qx[:, cols]
        lower = jnp.where(same, dot_nt(query_f, kf), dot_nt(query_f, kx))
        upper = jnp.where(same, dot_nt(query_b, kb), dot_nt(query_x, kb))
        scores = jnp.where(below, lower, upper).astype(bf16)
        acc[h] = jnp.dot(scores, v, preferred_element_type=f32)

    def piece(h, s):
        return pl.ds(h * DV + s * DVS, DVS)

    def middle(h):
        @pl.when(inner)
        def _():
            if h in STATES:
                landed(vcat.at[lo, vcols(h)], zrecv.at[VE + h])
            landed(ke.at[h], zrecv.at[KE + h])
            far_keys = ke[h]
            kcat[h, lo] = (far_keys.astype(f32) * rate[:, kcols(h)]).astype(bf16)
            if h in PAIRS:
                i = PAIRS.index(h)
                zput(kcat.at[h, lo], kin.at[i, hi], 1, KIN + 2 * i + 1, across)
            else:
                i = STATES.index(h)
                both = kcat[h]
                for s in range(SPLIT):
                    sbuf[i, s] = dot_tn(vcat[:, piece(h, s)], both).astype(bf16)
                    zput(sbuf.at[i, s], rbuf.at[i, s], 2, ST + i * SPLIT + s, across)
            seen = dot_nt(qs[side, h], far_keys).astype(bf16)
            acc[h] += jnp.dot(seen, vcat[lo, vcols(h)], preferred_element_type=f32)

    def serve(h):
        @pl.when(inner)
        def _():
            landed(qraw.at[h], zrecv.at[QE + h])
            raw = qraw[h]
            q2[h, lo] = qs[other, h]
            q2[h, hi] = (raw.astype(f32) * rate[:, kcols(h)]).astype(bf16)
            near = dot_nt(raw, knear[h]).astype(bf16)
            base[h] = jnp.dot(near, vcat[hi, vcols(h)], preferred_element_type=f32)

    def emit(h):
        cols = vcols(h)
        mixed = acc[h].astype(bf16).astype(f32)
        scale = lax.rsqrt(jnp.mean(mixed * mixed, axis=-1, keepdims=True) + norm_eps)
        outv[:, cols] = (mixed * scale * gain[:, cols]).astype(bf16)
        pltpu.make_async_copy(outv.at[:, cols], out.at[:, cols], osem.at[0]).start()

    def finish(h):
        @pl.when(inner)
        def _():
            if h in PAIRS:
                i = PAIRS.index(h)
                for part, where in enumerate((lo, hi)):
                    landed(vin.at[i, where], zrecv.at[VIN + 2 * i + part])
                    landed(kin.at[i, where], zrecv.at[KIN + 2 * i + part])
                seen = dot_nt(q2[h], kin[i]).astype(bf16)
            for s in range(SPLIT):
                cut = pl.ds(s * DVS, DVS)
                if h in PAIRS:
                    both = jnp.dot(seen, vin[i, :, cut], preferred_element_type=f32)
                else:
                    i = STATES.index(h)
                    landed(rbuf.at[i, s], zrecv.at[ST + i * SPLIT + s])
                    both = dot_nt(q2[h], rbuf[i, s])
                obuf[h, s] = (base[h, :, cut] + both[tok:]).astype(bf16)
                zput(obuf.at[h, s], oin.at[h, s], 3, h * SPLIT + s, mate)
                acc[h, :, cut] += both[:tok]

        @pl.when(edge)
        def _():
            for s in range(SPLIT):
                landed(oin.at[h, s], zrecv.at[h * SPLIT + s])
                acc[h, :, pl.ds(s * DVS, DVS)] += oin[h, s].astype(f32)

        emit(h)

    names = dict(
        prep=prep, first=wsend_first, rest=wsend_rest, relay=wrelay, hand=wpass, last=wlast, wall=wall,
        project=project, middle=middle, serve=serve, finish=finish, values=edge_values,
        queries=edge_queries, forward=vforward)
    loads[7].wait()
    for name, h in PLAN:
        names[name](h)

    gone(wbuf.at[:, pl.ds(0, n_dp - 1)], wsend.at[0])

    @pl.when(edge)
    def _():
        gone(vcat.at[hi], zsend.at[0])
        gone(qraw, zsend.at[1])
        gone(ke, zsend.at[2])

    @pl.when(inner)
    def _():
        gone(vin, zsend.at[0])
        gone(kin, zsend.at[1])
        gone(sbuf, zsend.at[2])
        gone(obuf, zsend.at[3])

    pltpu.make_async_copy(outv, out, osem.at[0]).wait()


def line_scratch(n_dp, tok, width, depth, rank):
    dma = pltpu.SemaphoreType.DMA
    v = pltpu.VMEM
    pairs, states = len(PAIRS), len(STATES)
    return [
        v((rank, width), bf16), v((rank, KEY), f32), v((1, KEY), f32), v((1, tok), bf16), v((1, VAL), f32),
        v((HEADS, n_dp, depth, DK), bf16),
        v((tok, width), bf16),
        v((tok, KEY), bf16),
        v((2 * tok, VAL), bf16),
        v((tok, VAL), bf16),
        v((tok, KEY), bf16), v((tok, KEY), bf16), v((tok, KEY), bf16),
        v((2, HEADS, tok, DK), bf16),
        v((5, tok, KEY), f32),
        v((1, KEY), f32),
        v((HEADS, tok, DV), f32),
        v((HEADS, tok, DV), f32),
        v((HEADS, 2 * tok, DK), bf16),
        v((HEADS, tok, DK), bf16),
        v((HEADS, 2 * tok, DK), bf16),
        v((HEADS, tok, DK), bf16),
        v((HEADS, tok, DK), bf16),
        v((pairs, 2 * tok, DV), bf16),
        v((pairs, 2 * tok, DK), bf16),
        v((states, SPLIT, DVS, DK), bf16),
        v((states, SPLIT, DVS, DK), bf16),
        v((HEADS, SPLIT, tok, DVS), bf16),
        v((HEADS, SPLIT, tok, DVS), bf16),
        dma((HEADS + 8,)),
        dma((1,)),
        dma((1,)),
        dma((HEADS, 2)),
        dma((HEADS,)),
        dma((HEADS,)),
        dma((HEADS,)),
        dma((4,)),
        dma((3 * HEADS + states * SPLIT + 4 * pairs,)),
    ]


def body(n_sp, n_dp, hidden, queries, values, key_weight, decay_down, decay_up, decay_bias,
         span_shift, norm_gain):
    seqs, length, width = hidden.shape
    tok = seqs * length
    assert tok == 2 * BLOCK
    chips = n_dp // CORES
    depth = key_weight.shape[0]
    anywhere = pl.BlockSpec(memory_space=pl.ANY)
    operands = (
        hidden.reshape(tok, width), queries.reshape(tok, KEY), values.reshape(tok, VAL),
        key_weight, decay_down.T, decay_up, decay_bias.reshape(1, KEY),
        span_shift.reshape(1, tok), norm_gain.reshape(1, VAL),
    )
    if n_sp == 4 and chips == 4:
        result = pl.pallas_call(
            functools.partial(line_kernel, n_sp, n_dp),
            out_shape=jax.ShapeDtypeStruct((tok, VAL), bf16),
            in_specs=[anywhere] * 9,
            out_specs=anywhere,
            scratch_shapes=line_scratch(n_dp, tok, width, depth, decay_up.shape[0]),
            compiler_params=pltpu.CompilerParams(
                collective_id=0, has_side_effects=True, vmem_limit_bytes=62 * 1024 * 1024),
        )(*operands)
        return result.reshape(seqs, length, VAL)
    vmem = pl.BlockSpec(memory_space=pltpu.VMEM)
    dma = pltpu.SemaphoreType.DMA
    result = pl.pallas_call(
        functools.partial(kernel, n_sp, n_dp),
        out_shape=jax.ShapeDtypeStruct((tok, VAL), bf16),
        in_specs=[anywhere] * 4 + [vmem] * 5,
        out_specs=anywhere,
        scratch_shapes=[
            pltpu.VMEM((HEADS, n_dp, depth, DK), bf16),
            pltpu.VMEM((tok, width), bf16),
            pltpu.VMEM((tok, KEY), bf16),
            pltpu.VMEM((tok, VAL), bf16),
            pltpu.VMEM((tok, VAL), bf16),
            pltpu.VMEM((tok, KEY), bf16),
            pltpu.VMEM((tok, KEY), bf16),
            pltpu.VMEM((tok, KEY), bf16),
            pltpu.VMEM((2, tok, KEY), bf16),
            pltpu.VMEM((5, tok, KEY), f32),
            pltpu.VMEM((1, KEY), f32),
            pltpu.VMEM((2, HEADS, DV, DK), f32),
            pltpu.VMEM((2, HEADS, SPLIT, DVS, DK), bf16),
            pltpu.VMEM((2, HEADS, SPLIT, DVS, DK), bf16),
            pltpu.VMEM((HEADS, tok, DV), f32),
            dma((HEADS + 3,)),
            dma((HEADS,)),
            dma((HEADS, chips)),
            dma((HEADS, chips)),
            dma((HEADS, chips)),
            dma((HEADS, chips)),
            dma((2, HEADS, SPLIT)),
            dma((2, HEADS, SPLIT)),
            dma((HEADS, 2)),
            dma((HEADS, 2)),
        ],
        compiler_params=pltpu.CompilerParams(
            collective_id=0, has_side_effects=True, vmem_limit_bytes=62 * 1024 * 1024),
    )(*operands)
    return result.reshape(seqs, length, VAL)


def solution(mesh):
    in_specs = (
        P("dp", "sp", None), P("dp", "sp", None), P("dp", "sp", None), P("dp", None),
        P(), P(), P(), P("dp", "sp"), P(),
    )
    return jax.shard_map(
        functools.partial(body, mesh.shape["sp"], mesh.shape["dp"]),
        mesh=mesh, in_specs=in_specs, out_specs=P("dp", "sp", None), check_vma=False)
```

```python
import functools

import jax
import jax.numpy as jnp
from jax import lax
from jax.experimental import pallas as pl
from jax.experimental.pallas import tpu as pltpu
from jax.sharding import PartitionSpec as P

HEADS = 4
DK = 256
DV = 512
BLOCK = 64
KEY = 1024
VAL = 2048
CORES = 2
SPLIT = 4
DVS = DV // SPLIT
STATES = (0, 1)
PAIRS = (2, 3)
EDGE_PLAN = (
    ("prep", 0), ("prep", 1), ("prep", 2), ("relay", 0), ("first", 1), ("rest", 1), ("first", 2),
    ("prep", 3), ("hand", 0), ("last", 0), ("wall", 0), ("project", 0), ("values", 1), ("queries", 0),
    ("relay", 1), ("rest", 2), ("first", 3), ("score", 0), ("hand", 1),
    ("relay", 2), ("rest", 3), ("last", 1), ("wall", 1), ("project", 1), ("queries", 1), ("queries", 2),
    ("hand", 2), ("score", 1), ("relay", 3), ("last", 2), ("wall", 2), ("project", 2), ("queries", 3),
    ("hand", 3), ("score", 2), ("last", 3), ("wall", 3), ("project", 3), ("score", 3),
    ("finish", 0), ("finish", 2), ("finish", 3), ("finish", 1),
)
INNER_PLAN = (
    ("prep", 0), ("prep", 1), ("prep", 2), ("relay", 0), ("first", 1), ("rest", 1), ("first", 2),
    ("prep", 3), ("hand", 0), ("forward", 2), ("last", 0), ("forward", 3), ("wall", 0), ("project", 0),
    ("relay", 1), ("rest", 2), ("first", 3), ("score", 0), ("hand", 1),
    ("relay", 2), ("rest", 3), ("middle", 0), ("push", 0, 0), ("push", 0, 1), ("push", 0, 2), ("push", 0, 3), ("cross", 0),
    ("last", 1), ("hand", 2), ("wall", 1), ("project", 1), ("score", 1),
    ("relay", 3), ("last", 2), ("middle", 1), ("push", 1, 0), ("push", 1, 1), ("cross", 1),
    ("serve", 0), ("wall", 2), ("project", 2), ("score", 2), ("hand", 3), ("last", 3),
    ("take", 0, 0), ("take", 0, 1), ("serve", 1), ("wall", 3), ("project", 3), ("middle", 2), ("score", 3), ("cross", 2),
    ("take", 0, 2), ("take", 0, 3), ("emit", 0), ("middle", 3), ("push", 1, 2), ("push", 1, 3), ("cross", 3),
    ("take", 1, 0), ("take", 1, 1),
    ("serve", 2), ("serve", 3), ("pair", 2), ("emit", 2), ("pair", 3), ("emit", 3), ("take", 1, 2), ("take", 1, 3), ("emit", 1),
)

decay_tau = 16.0
norm_eps = 1e-05
highest = lax.Precision.HIGHEST
MESH = pl.DeviceIdType.MESH
f32 = jnp.float32
bf16 = jnp.bfloat16


def each(low, high, fn):
    if high - low <= 4:
        for j in range(low, high):
            fn(j)
    else:
        lax.fori_loop(low, high, lambda j, c: (fn(j), c)[1], 0)


def dot_nt(a, b):
    return lax.dot_general(a, b, (((1,), (1,)), ((), ())), preferred_element_type=f32)


def dot_tn(a, b):
    return lax.dot_general(a, b, (((0,), (0,)), ((), ())), preferred_element_type=f32)


def kernel(
    n_sp, n_dp,
    hid, que, val, kw, down, up, bias, shift, gain,
    out,
    wbuf, hv, qv, vv, outv, qf, qb, qx, qs, fac, rate, local, sbuf, rbuf, acc,
    lsem, osem, wsend, wrecv, psend, precv, csend, crecv, dsend, drecv,
):
    sp = lax.axis_index("sp")
    dp = lax.axis_index("dp")
    chips = n_dp // CORES
    chip = dp // CORES
    core = dp % CORES
    partner = chip * CORES + (1 - core)
    tok = hv.shape[0]
    depth = kw.shape[0]

    square = chips == 4
    half = depth // 2

    def across(j):
        return (chip + 1 - 2 * lax.rem(chip, 2), lax.rem(chip + 2, 4), 3 - chip)[j - 1]

    def peer(j):
        if square:
            return across(j) * CORES + core
        return lax.rem(chip + j, chips) * CORES + core

    def source_chip(j):
        if square:
            return chip if j == 0 else across(j)
        return lax.rem(chip - j + chips, chips)

    wlocal = [
        pltpu.make_async_copy(kw.at[:, pl.ds(h * DK, DK)], wbuf.at[h, dp], lsem.at[h])
        for h in range(HEADS)
    ]
    inputs = [
        pltpu.make_async_copy(a, b, lsem.at[HEADS + i])
        for i, (a, b) in enumerate(((hid, hv), (que, qv), (val, vv)))
    ]
    for c in wlocal + inputs:
        c.start()

    barrier = pltpu.get_barrier_semaphore()
    each(1, chips, lambda j: pl.semaphore_signal(
        barrier, inc=1, device_id={"dp": peer(j)}, device_id_type=MESH))
    pl.semaphore_signal(barrier, inc=1, device_id={"dp": partner}, device_id_type=MESH)

    for side in (1, n_sp - 1):
        pl.semaphore_signal(
            barrier, inc=1, device_id={"sp": lax.rem(sp + side, n_sp)}, device_id_type=MESH)
    pl.semaphore_wait(barrier, chips + 2)

    def wcopy(h, j):
        return pltpu.make_async_remote_copy(
            src_ref=wbuf.at[h, dp], dst_ref=wbuf.at[h, dp],
            send_sem=wsend.at[h, j], recv_sem=wrecv.at[h, j],
            device_id={"dp": peer(j)}, device_id_type=MESH)

    def wland(h, j):
        slot = wbuf.at[h, source_chip(j) * CORES + core]
        return pltpu.make_async_remote_copy(
            src_ref=slot, dst_ref=slot,
            send_sem=wsend.at[h, j], recv_sem=wrecv.at[h, j],
            device_id={"dp": peer(j)}, device_id_type=MESH)

    def pcopy(h, j):
        slot = wbuf.at[h, source_chip(j) * CORES + core]
        return pltpu.make_async_remote_copy(
            src_ref=slot, dst_ref=slot,
            send_sem=psend.at[h, j], recv_sem=precv.at[h, j],
            device_id={"dp": partner}, device_id_type=MESH)

    def pland(h, j):
        slot = wbuf.at[h, source_chip(j) * CORES + (1 - core)]
        return pltpu.make_async_remote_copy(
            src_ref=slot, dst_ref=slot,
            send_sem=psend.at[h, j], recv_sem=precv.at[h, j],
            device_id={"dp": partner}, device_id_type=MESH)

    direct = 3 if square else chips

    def diagonal(h, i, lands):
        origin = source_chip(3) if lands else source_chip(1 + i)
        slot = wbuf.at[h, origin * CORES + core, pl.ds(i * half, half), :]
        return pltpu.make_async_remote_copy(
            src_ref=slot, dst_ref=slot,
            send_sem=dsend.at[h, i], recv_sem=drecv.at[h, i],
            device_id={"dp": peer(2 - i)}, device_id_type=MESH)

    def phase_send(h):
        wlocal[h].wait()
        each(1, direct, lambda j: wcopy(h, j).start())
        pcopy(h, 0).start()

    def phase_relay(h):
        def relay(j):
            wland(h, j).wait_recv()
            if square:
                diagonal(h, j - 1, False).start()
            pcopy(h, j).start()
        each(1, direct, relay)

    ahead = 2 if square else HEADS
    for h in range(ahead):
        phase_send(h)

    inputs[0].wait()
    low = dot_nt(hv[...], down[...]).astype(bf16)
    steps = shift[...].astype(f32)
    inputs[1].wait()
    row = lax.broadcasted_iota(jnp.int32, (tok, DK), 0)
    first = row < BLOCK
    ti = lax.broadcasted_iota(jnp.int32, (tok, tok), 0)
    tj = lax.broadcasted_iota(jnp.int32, (tok, tok), 1)
    same = (ti < BLOCK) == (tj < BLOCK)
    below = tj <= ti
    tri = jnp.where(same & below, 1.0, 0.0).astype(f32)
    def phase_prep(h):
        cols = pl.ds(h * DK, DK)
        pre = jnp.dot(low.astype(f32), up[:, cols], precision=highest, preferred_element_type=f32)
        pre = pre + bias[:, cols] + jnp.where(first, steps[:, :1], steps[:, BLOCK:BLOCK + 1])
        logd = (jnp.minimum(pre, 0.0) - jnp.log1p(jnp.exp(-jnp.abs(pre)))) * (1.0 / decay_tau)
        incl = jnp.dot(tri, logd, precision=highest, preferred_element_type=f32)
        excl = incl - logd
        t0 = incl[BLOCK - 1:BLOCK, :]
        t1 = incl[tok - 1:tok, :]
        here = jnp.where(first, t0, t1)
        after = jnp.where(first, t1, 0.0)
        before = jnp.where(first, 0.0, t0)
        scaled = qv[:, cols].astype(f32) * DK ** (-0.5)
        qf[:, cols] = (scaled * jnp.exp(incl)).astype(bf16)
        qb[:, cols] = (scaled * jnp.exp(-excl)).astype(bf16)
        qx[:, cols] = (scaled * jnp.exp(here - excl)).astype(bf16)
        qs[0, :, cols] = (scaled * jnp.exp(incl + before)).astype(bf16)
        qs[1, :, cols] = (scaled * jnp.exp(here - excl + after)).astype(bf16)
        fac[0, :, cols] = jnp.exp(-incl)
        fac[1, :, cols] = jnp.exp(excl)
        fac[2, :, cols] = jnp.exp(here - incl)
        fac[3, :, cols] = jnp.exp(here - incl + after)
        fac[4, :, cols] = jnp.exp(excl + before)
        rate[:, cols] = jnp.exp(t0 + t1)

    inputs[2].wait()

    def chain(way, h, s):
        target = jnp.clip(sp + 1 - 2 * way, 0, n_sp - 1)
        return pltpu.make_async_remote_copy(
            src_ref=sbuf.at[way, h, s], dst_ref=rbuf.at[way, h, s],
            send_sem=csend.at[way, h, s], recv_sem=crecv.at[way, h, s],
            device_id={"sp": target}, device_id_type=MESH)

    def phase_keys(h):
        if square:
            for i in range(2):
                diagonal(h, i, True).wait_recv()
            pcopy(h, 3).start()
        each(0, chips, lambda j: pland(h, j).wait_recv())
        cols = pl.ds(h * DK, DK)
        weights = wbuf[h].reshape(n_dp * depth, DK)
        keys = jnp.dot(hv[...], weights, preferred_element_type=f32).astype(bf16).astype(f32)
        v = vv[:, pl.ds(h * DV, DV)]
        k_fwd = (keys * fac[3, :, cols]).astype(bf16)
        k_bwd = (keys * fac[4, :, cols]).astype(bf16)
        for way, k in ((0, k_fwd), (1, k_bwd)):
            local[way, h] = dot_tn(v, k)

            @pl.when(sp == (0 if way == 0 else n_sp - 1))
            def _(way=way):
                for s in range(SPLIT):
                    sbuf[way, h, s] = local[way, h, pl.ds(s * DVS, DVS), :].astype(bf16)
                    chain(way, h, s).start()

        kf = (keys * fac[0, :, cols]).astype(bf16)
        kb = (keys * fac[1, :, cols]).astype(bf16)
        ke = (keys * fac[2, :, cols]).astype(bf16)
        query_f, query_b, query_x = qf[:, cols], qb[:, cols], qx[:, cols]
        lower = jnp.where(same, dot_nt(query_f, kf), dot_nt(query_f, ke))
        upper = jnp.where(same, dot_nt(query_b, kb), dot_nt(query_x, kb))
        scores = jnp.where(below, lower, upper).astype(bf16)
        acc[h] = jnp.dot(scores, v, preferred_element_type=f32)

    def phase_chain(way, h):
        cols = pl.ds(h * DK, DK)
        edge = way * (n_sp - 1)
        other = (1 - way) * (n_sp - 1)

        @pl.when(sp != edge)
        def _():
            for s in range(SPLIT):
                rows = pl.ds(s * DVS, DVS)
                chain(way, h, s).wait_recv()

                @pl.when(sp != other)
                def _(s=s, rows=rows):
                    state = rbuf[way, h, s].astype(f32) * rate[:, cols] + local[way, h, rows, :]
                    sbuf[way, h, s] = state.astype(bf16)
                    chain(way, h, s).start()

                acc[h, :, rows] += dot_nt(qs[way, :, cols], rbuf[way, h, s])

    def out_copy(h):
        cols = pl.ds(h * DV, DV)
        return pltpu.make_async_copy(outv.at[:, cols], out.at[:, cols], osem.at[h])

    def phase_out(h):
        cols = pl.ds(h * DV, DV)
        mixed = acc[h].astype(bf16).astype(f32)
        scale = lax.rsqrt(jnp.mean(mixed * mixed, axis=-1, keepdims=True) + norm_eps)
        outv[:, cols] = (mixed * scale * gain[:, cols]).astype(bf16)
        out_copy(h).start()

    near = jnp.where(sp * 2 < n_sp, 0, 1)
    far = 1 - near
    def relay_on(h):
        if h < HEADS:
            phase_relay(h)
            if h + ahead < HEADS:
                phase_send(h + ahead)

    def phase_near(h):
        phase_chain(near, h)

    def phase_far(h):
        phase_chain(far, h)
        phase_out(h)

    plan = ((phase_prep, 0), (relay_on, 0), (phase_prep, 1), (relay_on, 1), (phase_keys, 0), (phase_prep, 2), (relay_on, 2), (phase_keys, 1), (phase_prep, 3), (relay_on, 3), (phase_keys, 2), (phase_near, 0), (phase_keys, 3), (phase_near, 1), (phase_far, 0), (phase_near, 2), (phase_far, 1), (phase_near, 3), (phase_far, 2), (phase_far, 3))
    for phase, h in plan:
        phase(h)

    for h in range(HEADS):
        each(1, direct, lambda j, h=h: wcopy(h, j).wait_send())
        each(0, chips, lambda j, h=h: pcopy(h, j).wait_send())
        if square:
            for i in range(2):
                diagonal(h, i, False).wait_send()
        for way in range(2):
            @pl.when(sp != (1 - way) * (n_sp - 1))
            def _(h=h, way=way):
                for s in range(SPLIT):
                    chain(way, h, s).wait_send()
        out_copy(h).wait()


def line_kernel(
    n_sp, n_dp,
    hid, que, val, kw, down_in, up_in, bias_in, shift_in, gain_in,
    out,
    down, up, bias, shift, gain,
    wbuf, hv, qv, vcat, outv, own, qf, qb, qx, qs, fac, rate, acc, base,
    kcat, knear, q2, qraw, ke, vin, kin, sbuf, rbuf, obuf, oin,
    lsem, osem, wsend, wfirst, wrest, wdiag, wpart, zsend, zrecv,
):
    sp = lax.axis_index("sp")
    dp = lax.axis_index("dp")
    chip = dp // CORES
    core = dp % CORES
    partner = chip * CORES + (1 - core)
    tok = hv.shape[0]
    depth = kw.shape[0]
    half = depth // 2
    n_chips = n_dp // CORES

    side = sp // 2
    other = 1 - side
    mate = sp + 1 - 2 * lax.rem(sp, 2)
    across = n_sp - 1 - sp
    edge = (sp == 0) | (sp == n_sp - 1)
    inner = jnp.logical_not(edge)

    def chip_at(j):
        return (chip, chip + 1 - 2 * lax.rem(chip, 2), lax.rem(chip + 2, 4), 3 - chip)[j]

    def dev(j):
        return chip_at(j) * CORES + core

    wlocal = [
        pltpu.make_async_copy(kw.at[:, pl.ds(h * DK, DK)], wbuf.at[h, dp], lsem.at[h])
        for h in range(HEADS)
    ]
    loads = [
        pltpu.make_async_copy(a, b, lsem.at[HEADS + i])
        for i, (a, b) in enumerate((
            (hid, hv), (que, qv), (val, vcat.at[pl.ds(tok, tok)]),
            (down_in, down), (up_in, up), (bias_in, bias), (shift_in, shift), (gain_in, gain)))
    ]
    barrier = pltpu.get_barrier_semaphore()
    for j in (1, 2):
        pl.semaphore_signal(barrier, inc=1, device_id={"dp": dev(j)}, device_id_type=MESH)
    pl.semaphore_signal(barrier, inc=1, device_id={"dp": partner}, device_id_type=MESH)
    pl.semaphore_signal(barrier, inc=1, device_id={"sp": mate}, device_id_type=MESH)

    @pl.when(inner)
    def _():
        pl.semaphore_signal(barrier, inc=1, device_id={"sp": across}, device_id_type=MESH)

    wlocal[0].start()
    for i in (2, 0, 3, 4, 5, 6, 1):
        loads[i].start()
    for h in range(1, HEADS):
        wlocal[h].start()
    loads[7].start()
    pl.semaphore_wait(barrier, jnp.where(inner, 5, 4))

    def rows(i):
        return pl.ds(i * half, half)

    def wcopy(h, j, i):
        part = wbuf.at[h, dp, rows(i)]
        first = i == j - 1
        return pltpu.make_async_remote_copy(
            src_ref=part, dst_ref=part, send_sem=wsend.at[0],
            recv_sem=wfirst.at[h, i] if first else wrest.at[h],
            device_id={"dp": dev(j)}, device_id_type=MESH)

    def relay(h, i):
        part = wbuf.at[h, dev(1 + i), rows(i)]
        return pltpu.make_async_remote_copy(
            src_ref=part, dst_ref=part, send_sem=wsend.at[0], recv_sem=wdiag.at[h],
            device_id={"dp": dev(2 - i)}, device_id_type=MESH)

    def pcopy(h, j):
        slot = wbuf.at[h, dev(j)]
        return pltpu.make_async_remote_copy(
            src_ref=slot, dst_ref=slot, send_sem=wsend.at[0], recv_sem=wpart.at[h],
            device_id={"dp": partner}, device_id_type=MESH)

    def landed(ref, sem):
        pltpu.make_async_remote_copy(
            src_ref=ref, dst_ref=ref, send_sem=zsend.at[0], recv_sem=sem,
            device_id={"sp": mate}, device_id_type=MESH).wait_recv()

    def gone(ref, sem):
        pltpu.make_async_remote_copy(
            src_ref=ref, dst_ref=ref, send_sem=sem, recv_sem=zrecv.at[0],
            device_id={"sp": mate}, device_id_type=MESH).wait_send()

    def zput(src, dst, send, recv, target):
        pltpu.make_async_remote_copy(
            src_ref=src, dst_ref=dst, send_sem=zsend.at[send], recv_sem=zrecv.at[recv],
            device_id={"sp": target}, device_id_type=MESH).start()

    def wsend_first(h):
        wlocal[h].wait()
        for j in (1, 2):
            wcopy(h, j, j - 1).start()
        pcopy(h, 0).start()

    def wsend_rest(h):
        for j in (1, 2):
            wcopy(h, j, 2 - j).start()

    def wrelay(h):
        for i in range(2):
            landed(wbuf.at[h, dev(1 + i), rows(i)], wfirst.at[h, i])
            relay(h, i).start()

    def wpass(h):
        landed(wbuf.at[h, 0], wrest.at[h])
        for j in (1, 2):
            pcopy(h, j).start()

    def wlast(h):
        landed(wbuf.at[h, dev(3)], wdiag.at[h])
        pcopy(h, 3).start()

    def wall(h):
        landed(wbuf.at[h, pl.ds(0, n_chips)], wpart.at[h])

    VE, QE, KE = 0, HEADS, 2 * HEADS
    ST = 3 * HEADS
    VIN = ST + len(STATES) * SPLIT
    KIN = VIN + 2 * len(PAIRS)

    lo, hi = pl.ds(0, tok), pl.ds(tok, tok)

    def kcols(h):
        return pl.ds(h * DK, DK)

    def vcols(h):
        return pl.ds(h * DV, DV)

    def edge_values(h):
        zput(vcat.at[hi, vcols(h)], vcat.at[lo, vcols(h)], 0, VE + h, mate)

    def inner_values(h):
        zput(vcat.at[hi, vcols(h)], vin.at[PAIRS.index(h), lo], 0, VIN + 2 * PAIRS.index(h), across)

    def vforward(h):
        i = PAIRS.index(h)
        landed(vcat.at[lo, vcols(h)], zrecv.at[VE + h])
        zput(vcat.at[lo, vcols(h)], vin.at[i, hi], 0, VIN + 2 * i + 1, across)

    def edge_queries(h):
        zput(qs.at[other, h], qraw.at[h], 1, QE + h, mate)

    wsend_first(0)
    wsend_rest(0)
    loads[2].wait()

    @pl.when(inner)
    def _():
        for h in PAIRS:
            inner_values(h)

    @pl.when(edge)
    def _():
        for h in PAIRS + STATES[:1]:
            edge_values(h)

    for i in (0, 3):
        loads[i].wait()
    low = dot_nt(hv[...], down[...]).astype(bf16).astype(f32)
    for i in (4, 5, 6, 1):
        loads[i].wait()
    steps = shift[...].astype(f32)
    row = lax.broadcasted_iota(jnp.int32, (tok, DK), 0)
    first = row < BLOCK
    ti = lax.broadcasted_iota(jnp.int32, (tok, tok), 0)
    tj = lax.broadcasted_iota(jnp.int32, (tok, tok), 1)
    same = (ti < BLOCK) == (tj < BLOCK)
    below = tj <= ti
    tri = jnp.where(same & below, 1.0, 0.0).astype(f32)

    def prep(at_edge, h):
        cols = kcols(h)
        pre = jnp.dot(low, up[:, cols], precision=highest, preferred_element_type=f32)
        pre = pre + bias[:, cols] + jnp.where(first, steps[:, :1], steps[:, BLOCK:BLOCK + 1])
        logd = (jnp.minimum(pre, 0.0) - jnp.log1p(jnp.exp(-jnp.abs(pre)))) * (1.0 / decay_tau)
        incl = jnp.dot(tri, logd, precision=highest, preferred_element_type=f32)
        excl = incl - logd
        t0 = incl[BLOCK - 1:BLOCK, :]
        t1 = incl[tok - 1:tok, :]
        here = jnp.where(first, t0, t1)
        after = jnp.where(first, t1, 0.0)
        before = jnp.where(first, 0.0, t0)
        scaled = qv[:, cols].astype(f32) * DK ** (-0.5)
        qf[:, cols] = (scaled * jnp.exp(incl)).astype(bf16)
        qb[:, cols] = (scaled * jnp.exp(-excl)).astype(bf16)
        qx[:, cols] = (scaled * jnp.exp(here - excl)).astype(bf16)
        ahead, behind = incl + before, here - excl + after
        if at_edge:
            qs[other, h] = (scaled * jnp.exp(jnp.where(side == 1, ahead, behind))).astype(bf16)
        else:
            qs[0, h] = (scaled * jnp.exp(ahead)).astype(bf16)
            qs[1, h] = (scaled * jnp.exp(behind)).astype(bf16)
        fac[0, :, cols] = jnp.exp(-incl)
        fac[1, :, cols] = jnp.exp(excl)
        fac[2, :, cols] = jnp.exp(here - incl)
        ahead, behind = here - incl + after, excl + before
        if at_edge:
            fac[3 + side, :, cols] = jnp.exp(jnp.where(side == 0, ahead, behind))
        else:
            fac[3, :, cols] = jnp.exp(ahead)
            fac[4, :, cols] = jnp.exp(behind)
            rate[:, cols] = jnp.exp(t0 + t1)

    def project(at_edge, h):
        cols = kcols(h)
        weights = wbuf[h].reshape(n_dp * depth, DK)
        keys = jnp.dot(hv[...], weights, preferred_element_type=f32).astype(bf16)
        own[:, cols] = keys
        keys = keys.astype(f32)
        kcat[h, hi] = (keys * fac[3 + side, :, cols]).astype(bf16)
        if at_edge:
            zput(kcat.at[h, hi], ke.at[h], 2, KE + h, mate)
        elif h in PAIRS:
            i = PAIRS.index(h)
            zput(kcat.at[h, hi], kin.at[i, lo], 1, KIN + 2 * i, across)

    def score(at_edge, h):
        cols = kcols(h)
        keys = own[:, cols].astype(f32)
        if not at_edge:
            knear[h] = (keys * fac[3 + other, :, cols]).astype(bf16)
        v = vcat[hi, vcols(h)]
        kf = (keys * fac[0, :, cols]).astype(bf16)
        kb = (keys * fac[1, :, cols]).astype(bf16)
        kx = (keys * fac[2, :, cols]).astype(bf16)
        query_f, query_b, query_x = qf[:, cols], qb[:, cols], qx[:, cols]
        lower = jnp.where(same, dot_nt(query_f, kf), dot_nt(query_f, kx))
        upper = jnp.where(same, dot_nt(query_b, kb), dot_nt(query_x, kb))
        scores = jnp.where(below, lower, upper).astype(bf16)
        acc[h] = jnp.dot(scores, v, preferred_element_type=f32)

    def piece(h, s):
        return pl.ds(h * DV + s * DVS, DVS)

    def middle(h):
        if h in STATES:
            landed(vcat.at[lo, vcols(h)], zrecv.at[VE + h])
        landed(ke.at[h], zrecv.at[KE + h])
        far_keys = ke[h]
        kcat[h, lo] = (far_keys.astype(f32) * rate[:, kcols(h)]).astype(bf16)
        if h in PAIRS:
            i = PAIRS.index(h)
            zput(kcat.at[h, lo], kin.at[i, hi], 1, KIN + 2 * i + 1, across)
        else:
            i = STATES.index(h)
            both = kcat[h]
            for s in range(SPLIT):
                sbuf[i, s] = dot_tn(vcat[:, piece(h, s)], both).astype(bf16)

    def push(h, s):
        i = STATES.index(h)
        zput(sbuf.at[i, s], rbuf.at[i, s], 2, ST + i * SPLIT + s, across)

    def cross(h):
        seen = dot_nt(qs[side, h], ke[h]).astype(bf16)
        acc[h] += jnp.dot(seen, vcat[lo, vcols(h)], preferred_element_type=f32)

    def serve(h):
        landed(qraw.at[h], zrecv.at[QE + h])
        raw = qraw[h]
        q2[h, lo] = qs[other, h]
        q2[h, hi] = (raw.astype(f32) * rate[:, kcols(h)]).astype(bf16)
        near = dot_nt(raw, knear[h]).astype(bf16)
        base[h] = jnp.dot(near, vcat[hi, vcols(h)], preferred_element_type=f32)

    def emit(h):
        cols = vcols(h)
        mixed = acc[h].astype(bf16).astype(f32)
        scale = lax.rsqrt(jnp.mean(mixed * mixed, axis=-1, keepdims=True) + norm_eps)
        outv[:, cols] = (mixed * scale * gain[:, cols]).astype(bf16)
        pltpu.make_async_copy(outv.at[:, cols], out.at[:, cols], osem.at[0]).start()

    def share(h, s, both):
        cut = pl.ds(s * DVS, DVS)
        obuf[h, s] = (base[h, :, cut] + both[tok:]).astype(bf16)
        zput(obuf.at[h, s], oin.at[h, s], 3, h * SPLIT + s, mate)
        acc[h, :, cut] += both[:tok]

    def take(h, s):
        i = STATES.index(h)
        landed(rbuf.at[i, s], zrecv.at[ST + i * SPLIT + s])
        share(h, s, dot_nt(q2[h], rbuf[i, s]))

    def pair(h):
        i = PAIRS.index(h)
        for part, where in enumerate((lo, hi)):
            landed(vin.at[i, where], zrecv.at[VIN + 2 * i + part])
            landed(kin.at[i, where], zrecv.at[KIN + 2 * i + part])
        seen = dot_nt(q2[h], kin[i]).astype(bf16)
        for s in range(SPLIT):
            share(h, s, jnp.dot(seen, vin[i, :, pl.ds(s * DVS, DVS)], preferred_element_type=f32))

    def finish(h):
        for s in range(SPLIT):
            landed(oin.at[h, s], zrecv.at[h * SPLIT + s])
            acc[h, :, pl.ds(s * DVS, DVS)] += oin[h, s].astype(f32)
        emit(h)

    loads[7].wait()

    def run(at_edge, plan):
        names = dict(
            prep=functools.partial(prep, at_edge), first=wsend_first, rest=wsend_rest, relay=wrelay,
            hand=wpass, last=wlast, wall=wall, project=functools.partial(project, at_edge),
            score=functools.partial(score, at_edge), middle=middle, serve=serve,
            push=push, cross=cross, take=take, pair=pair, emit=emit, finish=finish, values=edge_values, queries=edge_queries,
            forward=vforward)
        for name, *where in plan:
            names[name](*where)

    @pl.when(edge)
    def _():
        run(True, EDGE_PLAN)

    @pl.when(inner)
    def _():
        run(False, INNER_PLAN)

    gone(wbuf.at[:, pl.ds(0, n_dp - 1)], wsend.at[0])

    @pl.when(edge)
    def _():
        gone(vcat.at[hi], zsend.at[0])
        gone(qraw, zsend.at[1])
        gone(ke, zsend.at[2])

    @pl.when(inner)
    def _():
        gone(vin, zsend.at[0])
        gone(kin, zsend.at[1])
        gone(sbuf, zsend.at[2])
        gone(obuf, zsend.at[3])

    pltpu.make_async_copy(outv, out, osem.at[0]).wait()


def line_scratch(n_dp, tok, width, depth, rank):
    dma = pltpu.SemaphoreType.DMA
    v = pltpu.VMEM
    pairs, states = len(PAIRS), len(STATES)
    return [
        v((rank, width), bf16), v((rank, KEY), f32), v((1, KEY), f32), v((1, tok), bf16), v((1, VAL), f32),
        v((HEADS, n_dp, depth, DK), bf16),
        v((tok, width), bf16),
        v((tok, KEY), bf16),
        v((2 * tok, VAL), bf16),
        v((tok, VAL), bf16),
        v((tok, KEY), bf16), v((tok, KEY), bf16), v((tok, KEY), bf16), v((tok, KEY), bf16),
        v((2, HEADS, tok, DK), bf16),
        v((5, tok, KEY), f32),
        v((1, KEY), f32),
        v((HEADS, tok, DV), f32),
        v((HEADS, tok, DV), f32),
        v((HEADS, 2 * tok, DK), bf16),
        v((HEADS, tok, DK), bf16),
        v((HEADS, 2 * tok, DK), bf16),
        v((HEADS, tok, DK), bf16),
        v((HEADS, tok, DK), bf16),
        v((pairs, 2 * tok, DV), bf16),
        v((pairs, 2 * tok, DK), bf16),
        v((states, SPLIT, DVS, DK), bf16),
        v((states, SPLIT, DVS, DK), bf16),
        v((HEADS, SPLIT, tok, DVS), bf16),
        v((HEADS, SPLIT, tok, DVS), bf16),
        dma((HEADS + 8,)),
        dma((1,)),
        dma((1,)),
        dma((HEADS, 2)),
        dma((HEADS,)),
        dma((HEADS,)),
        dma((HEADS,)),
        dma((4,)),
        dma((3 * HEADS + states * SPLIT + 4 * pairs,)),
    ]


def body(n_sp, n_dp, hidden, queries, values, key_weight, decay_down, decay_up, decay_bias,
         span_shift, norm_gain):
    seqs, length, width = hidden.shape
    tok = seqs * length
    assert tok == 2 * BLOCK
    chips = n_dp // CORES
    depth = key_weight.shape[0]
    anywhere = pl.BlockSpec(memory_space=pl.ANY)
    operands = (
        hidden.reshape(tok, width), queries.reshape(tok, KEY), values.reshape(tok, VAL),
        key_weight, decay_down.T, decay_up, decay_bias.reshape(1, KEY),
        span_shift.reshape(1, tok), norm_gain.reshape(1, VAL),
    )
    if n_sp == 4 and chips == 4:
        result = pl.pallas_call(
            functools.partial(line_kernel, n_sp, n_dp),
            out_shape=jax.ShapeDtypeStruct((tok, VAL), bf16),
            in_specs=[anywhere] * 9,
            out_specs=anywhere,
            scratch_shapes=line_scratch(n_dp, tok, width, depth, decay_up.shape[0]),
            compiler_params=pltpu.CompilerParams(
                collective_id=0, has_side_effects=True, vmem_limit_bytes=62 * 1024 * 1024),
        )(*operands)
        return result.reshape(seqs, length, VAL)
    vmem = pl.BlockSpec(memory_space=pltpu.VMEM)
    dma = pltpu.SemaphoreType.DMA
    result = pl.pallas_call(
        functools.partial(kernel, n_sp, n_dp),
        out_shape=jax.ShapeDtypeStruct((tok, VAL), bf16),
        in_specs=[anywhere] * 4 + [vmem] * 5,
        out_specs=anywhere,
        scratch_shapes=[
            pltpu.VMEM((HEADS, n_dp, depth, DK), bf16),
            pltpu.VMEM((tok, width), bf16),
            pltpu.VMEM((tok, KEY), bf16),
            pltpu.VMEM((tok, VAL), bf16),
            pltpu.VMEM((tok, VAL), bf16),
            pltpu.VMEM((tok, KEY), bf16),
            pltpu.VMEM((tok, KEY), bf16),
            pltpu.VMEM((tok, KEY), bf16),
            pltpu.VMEM((2, tok, KEY), bf16),
            pltpu.VMEM((5, tok, KEY), f32),
            pltpu.VMEM((1, KEY), f32),
            pltpu.VMEM((2, HEADS, DV, DK), f32),
            pltpu.VMEM((2, HEADS, SPLIT, DVS, DK), bf16),
            pltpu.VMEM((2, HEADS, SPLIT, DVS, DK), bf16),
            pltpu.VMEM((HEADS, tok, DV), f32),
            dma((HEADS + 3,)),
            dma((HEADS,)),
            dma((HEADS, chips)),
            dma((HEADS, chips)),
            dma((HEADS, chips)),
            dma((HEADS, chips)),
            dma((2, HEADS, SPLIT)),
            dma((2, HEADS, SPLIT)),
            dma((HEADS, 2)),
            dma((HEADS, 2)),
        ],
        compiler_params=pltpu.CompilerParams(
            collective_id=0, has_side_effects=True, vmem_limit_bytes=62 * 1024 * 1024),
    )(*operands)
    return result.reshape(seqs, length, VAL)


def solution(mesh):
    in_specs = (
        P("dp", "sp", None), P("dp", "sp", None), P("dp", "sp", None), P("dp", None),
        P(), P(), P(), P("dp", "sp"), P(),
    )
    return jax.shard_map(
        functools.partial(body, mesh.shape["sp"], mesh.shape["dp"]),
        mesh=mesh, in_specs=in_specs, out_specs=P("dp", "sp", None), check_vma=False)
```
